512 devices in a mesh: sp: 64 (over z, y), dp: 8 (over x, core).
Axes of the slice: x: 4, y: 8, z: 8, core: 2. Of those that a mesh axis runs over, the one named last changes fastest.
Arguments:
- inputs: bfloat16 [8, 8192, 2048], P('dp', 'sp'), may hold values from -6 to 6
- conv_weight: bfloat16 [4, 2048], replicated, may hold values from -3 to 3
- gate_weight: bfloat16 [2, 8, 256, 256], P(None, 'dp'), may hold values from -0.375 to 0.375
- rate_param: float32 [2048], replicated, may hold values from 4 to 12.5
- pace: float32 [8, 8192], P('dp'), may hold values from 0.5 to 30000
Outputs:
- recurrent: bfloat16 [8, 8192, 2048], P('dp', 'sp')
The draws below stay inside these ranges and needn't reach their ends.
All inputs are finite; a program needn't handle non-finite values.
Results may differ from the reference program's by a relative error of at most 0.008.
Values may be sent and summed in bfloat16 or wider, within the bound.
No kernel may reach another device: no remote copies, remote signals or barrier semaphores. Data moves between devices by JAX's collectives and lax.ppermute only.
A program may use at most 128 MiB of HBM per device.

```python
import math
import jax
import jax.numpy as jnp
from jax import lax

TOK_DEV = 128
HEADS = 8
BLOCK = 256
CONV = 4
DR = 2048
SEQUENCE_COUNT = 8
SEQUENCE_LENGTH = 8192


def draw_rate_param(key, part):
    slow_share = 0.5
    slow_mask = jax.random.uniform(jax.random.fold_in(key, 21), (HEADS * BLOCK,), jnp.float32) < slow_share
    slow_value = jax.random.uniform(jax.random.fold_in(key, 22), (HEADS * BLOCK,), jnp.float32, 11.5, 12.5)
    fast_value = jax.random.uniform(jax.random.fold_in(key, 23), (HEADS * BLOCK,), jnp.float32, 4.0, 6.0)
    return jnp.where(slow_mask, slow_value, fast_value)


def draw_pace(key, part):
    block_count = SEQUENCE_LENGTH // TOK_DEV
    factor = jnp.exp(jax.random.uniform(jax.random.fold_in(key, 11), (SEQUENCE_COUNT, block_count), jnp.float32, math.log(0.5), math.log(2.0)))
    constant_level = jnp.repeat(factor, TOK_DEV, axis=1)
    surge_position = jax.random.randint(jax.random.fold_in(key, 12), (SEQUENCE_COUNT, 3), 0, SEQUENCE_LENGTH)
    surge_length = jax.random.uniform(jax.random.fold_in(key, 13), (SEQUENCE_COUNT, 3), jnp.float32, 6000.0, 10000.0)
    position_flags = jnp.arange(SEQUENCE_LENGTH, dtype=jnp.int32)[None, None, :] == surge_position[:, :, None]
    surge_spans = jnp.sum(jnp.where(position_flags, surge_length[:, :, None], 0.0), axis=1)
    return constant_level + surge_spans


def shard_levels(own_key, dims, split, least, largest):
    def one(axis_at, shards_of):
        draws = jax.random.uniform(jax.random.fold_in(jax.random.fold_in(own_key, 6), axis_at), (shards_of,), jnp.float32, least / len(split), largest / len(split))
        return jnp.repeat(jnp.exp(draws), dims[axis_at] // shards_of).reshape((-1,) + (1,) * (len(dims) - axis_at - 1))

    factor_of = one(*split[0])
    for cut in split[1:]:
        factor_of = factor_of * one(*cut)
    return factor_of


def bell_draw(stream_key, shape, scale, most, split=(), kind=jnp.bfloat16):
    values = jax.random.normal(stream_key, shape, jnp.float32) * scale
    if len(split) > 0:
        values = shard_levels(stream_key, shape, split, -0.22, 0.18) * values
    return jnp.clip(values, min=-most, max=most).astype(kind)


def setup_inputs(seed: int = 0) -> dict:
    keys = jax.random.split(jax.random.key(seed), 6)
    inputs = bell_draw(keys[0], (SEQUENCE_COUNT, SEQUENCE_LENGTH, DR), 1.0, 6.0, ((0, 8), (1, 64)))
    conv_weight = bell_draw(keys[1], (CONV, DR), CONV ** -0.5, 3.0)
    gate_weight = bell_draw(keys[2], (2, HEADS, BLOCK, BLOCK), BLOCK ** -0.5, 0.375, ((1, 8),))
    rate_param = draw_rate_param(jax.random.fold_in(keys[5], 71), 0)
    pace = draw_pace(jax.random.fold_in(keys[5], 71), 0)
    return {"inputs": inputs, "conv_weight": conv_weight, "gate_weight": gate_weight, "rate_param": rate_param, "pace": pace}


gate_power = 8.0

def combine(earlier, later):
    decay_e, state_e = earlier
    decay_l, state_l = later
    return (decay_e * decay_l, decay_l * state_e + state_l)

def lru_terms(pre_recur, pre_input, values, rate_col, pace_col):
    recur_gate = jax.nn.sigmoid(pre_recur.astype(jnp.float32))
    input_gate = jax.nn.sigmoid(pre_input.astype(jnp.float32))
    log_decay = -gate_power * pace_col * recur_gate * jax.nn.softplus(-rate_col)
    decay = jnp.exp(log_decay)
    drive = jnp.sqrt(-jnp.expm1(2.0 * log_decay)) * input_gate * values.astype(jnp.float32)
    return (decay, drive)

def reference(inputs, conv_weight, gate_weight, rate_param, pace):

    def one_sequence(pair):
        seq_rows, seq_pace = pair
        length = seq_rows.shape[0]
        padded = jnp.pad(seq_rows.astype(jnp.float32), ((CONV - 1, 0), (0, 0)))
        conv_taps = conv_weight.astype(jnp.float32)
        conv_out = jnp.zeros((length, seq_rows.shape[1]), jnp.float32)
        for tap in range(CONV):
            conv_out = conv_out + conv_taps[tap][None, :] * padded[tap:tap + length]
        conv_out = conv_out.astype(jnp.bfloat16)
        by_head = conv_out.reshape(length, HEADS, BLOCK).transpose(1, 0, 2)
        head_weights = gate_weight.transpose(1, 0, 2, 3)
        head_rates = rate_param.reshape(HEADS, BLOCK)

        def one_head(triple):
            head_rows, weights, rates = triple
            preact = jnp.einsum('ti,gij->gtj', head_rows.astype(jnp.float32), weights.astype(jnp.float32)).astype(jnp.bfloat16)
            decay, drive = lru_terms(preact[0], preact[1], head_rows, rates[None, :], seq_pace[:, None])
            _, state = lax.associative_scan(combine, (decay, drive), axis=0)
            return state.astype(jnp.bfloat16)
        states = lax.map(one_head, (by_head, head_weights, head_rates))
        return states.transpose(1, 0, 2).reshape(length, HEADS * BLOCK)
    return lax.map(one_sequence, (inputs, pace))
```

```python
import functools

import jax
import jax.numpy as jnp
from jax import lax
from jax.experimental import pallas as pl
from jax.experimental.pallas import tpu as pltpu
from jax.sharding import Mesh
from jax.sharding import PartitionSpec as P

HEADS = 8
BLOCK = 256
CONV = 4
ROWS = 128
CHUNKS = 8
STEPS = ROWS // CHUNKS
LANES = 128

gate_power = 8.0
f32, bf16 = jnp.float32, jnp.bfloat16


def order_matrix(transposed):
    here = lax.broadcasted_iota(jnp.int32, (ROWS, ROWS), 1 if transposed else 0)
    position = lax.broadcasted_iota(jnp.int32, (ROWS, ROWS), 0 if transposed else 1)
    return position == (here & (CHUNKS - 1)) * STEPS + (here >> 3)


def softplus_of_minus(rate):
    e = jnp.exp(-jnp.abs(rate))
    series = e * (1 - e * (1 / 2 - e * (1 / 3 - e * (1 / 4 - e * (1 / 5 - e * (1 / 6))))))
    return jnp.maximum(-rate, 0.0) + jnp.where(e < 0.05, series, jnp.log(1.0 + e))


def sublane_before(tile, shift, fill):
    row = lax.broadcasted_iota(jnp.int32, tile.shape, 0)
    return jnp.where(row < shift, fill, pltpu.roll(tile, shift, 0))


def conv_all(x_ref, halo_ref, cw_ref, cv_ref):
    perm = order_matrix(False).astype(bf16)
    for h in range(HEADS):
        cols = pl.ds(h * BLOCK, BLOCK)
        moved = jnp.dot(perm, x_ref[:, cols], preferred_element_type=f32)
        step = [moved[CHUNKS * r : CHUNKS * (r + 1)] for r in range(STEPS)]
        halo = halo_ref[:, cols].astype(f32)
        taps = cw_ref[:, cols].astype(f32)
        early = [
            sublane_before(step[STEPS - j], 1, halo[8 - j : 9 - j]) for j in (3, 2, 1)
        ]
        line = early + step
        for r in range(0, STEPS, 2):
            both = []
            for q in (r, r + 1):
                total = taps[0:1] * line[q]
                for tap in range(1, CONV):
                    total = total + taps[tap : tap + 1] * line[q + tap]
                both.append(total)
            cv_ref[pl.ds(CHUNKS * r, 2 * CHUNKS), cols] = jnp.concatenate(both, 0).astype(bf16)


def one_head(head, cv_ref, w0, w1, pace_ref, rate_ref, pre_ref, h_ref, p_ref, edge_ref, slot):
    cols = pl.ds(pl.multiple_of(head * BLOCK, BLOCK), BLOCK)
    values = cv_ref[:, cols]
    pre_ref[0] = jnp.dot(values, w0, preferred_element_type=f32)
    pre_ref[1] = jnp.dot(values, w1, preferred_element_type=f32)
    pre_ref[2] = values.astype(f32)
    soft = gate_power * softplus_of_minus(rate_ref[:, cols])
    totals = []
    for lane in range(0, BLOCK, LANES):
        at = slice(lane, lane + LANES)
        soft_here = soft[:, at]
        state = run = used = None
        for r in range(STEPS):
            rows = slice(CHUNKS * r, CHUNKS * (r + 1))
            x0 = pre_ref[0, rows, at].astype(bf16).astype(f32)
            x1 = pre_ref[1, rows, at].astype(bf16).astype(f32)
            recur_gate = 1.0 / (1.0 + jnp.exp(-x0))
            input_gate = 1.0 / (1.0 + jnp.exp(-x1))
            loss = pace_ref[rows, :] * recur_gate * soft_here
            decay = jnp.exp(-loss)
            v = 2.0 * loss
            series = v * (1 - v * (1 / 2 - v * (1 / 6 - v * (1 / 24 - v * (1 / 120)))))
            gone = jnp.where(v < 0.1, series, 1.0 - decay * decay)
            drive = jnp.sqrt(gone) * input_gate * pre_ref[2, rows, at]
            if r == 0:
                state, run, used = drive, decay, loss
            else:
                state, run, used = decay * state + drive, decay * run, used + loss
            h_ref[slot, rows, at] = state
            p_ref[slot, rows, at] = run
        for shift in (1, 2, 4):
            state = state + run * sublane_before(state, shift, 0.0)
            run = run * sublane_before(run, shift, 1.0)
        edge_ref[slot, 0, :, at] = sublane_before(state, 1, 0.0)
        edge_ref[slot, 1, :, at] = sublane_before(run, 1, 1.0)
        totals.append((jnp.sum(used, 0, keepdims=True), state[CHUNKS - 1 : CHUNKS]))
    return tuple(jnp.concatenate([t[k] for t in totals], 1) for k in (0, 1))


def chips():
    x, c = lax.axis_index("dp_0"), lax.axis_index("dp_1")
    near = jnp.where(c == 0, x + 3, x + 1) & 3
    other = jnp.where(c == 0, x + 1, x + 3) & 3
    return x, c, near, other, (x + 2) & 3


def heads_of(group):
    x, c, near, other, far = chips()
    return {
        "own": [2 * x, 2 * x + 1],
        "near": [2 * near, 2 * near + 1, 2 * far + c],
        "rest": [2 * other, 2 * other + 1, 2 * far + 1 - c],
    }[group]


def own_kernel(x_ref, halo_ref, cw_ref, rate_ref, pace_ref, w_ref, cv_ref, pcol_ref, h_ref, p_ref, edge_ref, tot_ref, pre_ref):
    here = lax.axis_index("sp")
    pace = pace_ref[:, pl.ds(pl.multiple_of(here * ROWS, ROWS), ROWS)]
    column = jnp.sum(jnp.where(order_matrix(False), pace, 0.0), axis=1, keepdims=True)
    pcol_ref[...] = jnp.broadcast_to(column, (ROWS, LANES))
    conv_all(x_ref, halo_ref, cw_ref, cv_ref)
    for slot, head in enumerate(heads_of("own")):
        used, state = one_head(head, cv_ref, w_ref[slot, 0], w_ref[slot, 1], pcol_ref, rate_ref, pre_ref, h_ref, p_ref, edge_ref, slot)
        tot_ref[0, slot : slot + 1] = used
        tot_ref[1, slot : slot + 1] = state


def near_kernel(cv_ref, pcol_ref, rate_ref, wa_ref, wb_ref, h_ref, p_ref, edge_ref, tot_ref, pre_ref):
    for slot, head in enumerate(heads_of("near")):
        w = wb_ref if slot == 2 else wa_ref.at[slot]
        used, state = one_head(head, cv_ref, w[0], w[1], pcol_ref, rate_ref, pre_ref, h_ref, p_ref, edge_ref, slot)
        tot_ref[0, slot : slot + 1] = used
        tot_ref[1, slot : slot + 1] = state


def rest_kernel(cv_ref, pcol_ref, rate_ref, wa_ref, wb_ref, own_ref, near_ref, h_ref, p_ref, edge_ref, send_ref, pre_ref):
    totals = []
    for slot, head in enumerate(heads_of("rest")):
        w = wb_ref if slot == 2 else wa_ref.at[slot]
        totals.append(one_head(head, cv_ref, w[0], w[1], pcol_ref, rate_ref, pre_ref, h_ref, p_ref, edge_ref, slot))
    lines = []
    for k in (0, 1):
        lines += [own_ref[k, 0:2], near_ref[k, 0:3]] + [t[k] for t in totals]
    message = jnp.concatenate(lines, 0).astype(bf16)

    def put(j, _):
        send_ref[j] = message
        return 0

    lax.fori_loop(0, send_ref.shape[0], put, 0, unroll=8)


def last_kernel(all_ref, *refs):
    groups, out_ref = refs[:9], refs[9]
    here = lax.axis_index("sp")
    count = all_ref.shape[0]
    parts = []
    for first in range(0, count, 8):
        state = run = None
        for j in range(first, first + 8):
            line = all_ref[j].astype(f32)
            mine = (j < here).astype(f32)
            decay = jnp.exp(-(line[:HEADS] * mine))
            drive = line[HEADS:] * mine
            if state is None:
                state, run = drive, decay
            else:
                state, run = decay * state + drive, decay * run
        parts.append((run, state))
    carried = parts[0][1]
    for run, state in parts[1:]:
        carried = run * carried + state
    back = order_matrix(True).astype(bf16)
    at = 0
    for g, name in enumerate(("own", "near", "rest")):
        h_ref, p_ref, edge_ref = groups[3 * g : 3 * g + 3]
        for slot, head in enumerate(heads_of(name)):
            enters = edge_ref[slot, 0] + edge_ref[slot, 1] * carried[at : at + 1]
            whole = h_ref[slot].reshape(STEPS, CHUNKS, BLOCK) + p_ref[slot].reshape(
                STEPS, CHUNKS, BLOCK
            ) * enters.reshape(1, CHUNKS, BLOCK)
            rounded = whole.reshape(ROWS, BLOCK).astype(bf16)
            cols = pl.ds(pl.multiple_of(head * BLOCK, BLOCK), BLOCK)
            out_ref[:, cols] = jnp.dot(back, rounded, preferred_element_type=f32).astype(bf16)
            at += 1


def vmem(count):
    return [pl.BlockSpec(memory_space=pltpu.VMEM)] * count


def call(kernel, outs, args, name, scratch=True, us=2.0):
    return pl.pallas_call(
        kernel,
        name=name,
        out_shape=[jax.ShapeDtypeStruct(s, d) for s, d in outs],
        in_specs=vmem(len(args)),
        out_specs=vmem(len(outs)),
        scratch_shapes=[pltpu.VMEM((3, ROWS, BLOCK), f32)] if scratch else [],
        compiler_params=pltpu.CompilerParams(vmem_limit_bytes=16 * 2**20),
        cost_estimate=pl.CostEstimate(flops=int(us * 2e8), bytes_accessed=1 << 20, transcendentals=1 << 18),
    )(*args)


def head_outs(n):
    return [((n, ROWS, BLOCK), f32), ((n, ROWS, BLOCK), f32), ((n, 2, CHUNKS, BLOCK), f32)]


def body(inputs, conv_weight, gate_weight, rate_param, pace):
    x = inputs[0]
    rate = rate_param[None]
    devices = lax.axis_size("sp")
    dp = ("dp_0", "dp_1")
    core = [(0, 1), (1, 0)]
    own = gate_weight[:, 0]
    pair = lax.all_gather(own, "dp_1")
    near = lax.ppermute(
        pair, dp, [(2 * i + k, 2 * ((i + (1, 3)[k]) % 4) + k) for i in range(4) for k in (0, 1)]
    )
    far = lax.ppermute(own, "dp_0", [(i, (i + 2) % 4) for i in range(4)])
    halo = lax.ppermute(x[ROWS - 8 :], "sp", [(i, i + 1) for i in range(devices - 1)])
    cv, pcol, *own_out, own_tot = call(
        own_kernel,
        [((ROWS, HEADS * BLOCK), bf16), ((ROWS, LANES), f32), *head_outs(2), ((2, 2, BLOCK), f32)],
        (x, halo, conv_weight, rate, pace, pair),
        "own_heads",
    )
    other = lax.ppermute(near, "dp_1", core)
    other_far = lax.ppermute(far, "dp_1", core)
    *near_out, near_tot = call(
        near_kernel,
        [*head_outs(3), ((2, 3, BLOCK), f32)],
        (cv, pcol, rate, near, far),
        "near_heads",
    )
    *rest_out, send = call(
        rest_kernel,
        [*head_outs(3), ((devices, 2 * HEADS, BLOCK), bf16)],
        (cv, pcol, rate, other, other_far, own_tot, near_tot),
        "rest_heads",
    )
    everyone = lax.all_to_all(send, "sp", split_axis=0, concat_axis=0, tiled=True)
    (result,) = call(
        last_kernel,
        [((ROWS, HEADS * BLOCK), bf16)],
        (everyone, *own_out, *near_out, *rest_out),
        "carry_in",
        scratch=False,
    )
    return result[None]


def solution(mesh):
    finer = Mesh(mesh.devices.reshape(mesh.shape["sp"], 4, 2), ("sp", "dp_0", "dp_1"))
    dp = ("dp_0", "dp_1")
    in_specs = (P(dp, "sp", None), P(), P(None, dp, None, None), P(), P(dp, None))
    out_specs = P(dp, "sp", None)
    return jax.shard_map(body, mesh=finer, in_specs=in_specs, out_specs=out_specs, check_vma=False)
```

```python
import jax
import jax.numpy as jnp
from jax import lax
from jax.experimental import pallas as pl
from jax.experimental.pallas import tpu as pltpu
from jax.sharding import Mesh
from jax.sharding import PartitionSpec as P

HEADS = 8
BLOCK = 256
CONV = 4
ROWS = 128
CHUNKS = 8
STEPS = ROWS // CHUNKS
LANES = 128

gate_power = 8.0
f32, bf16 = jnp.float32, jnp.bfloat16


def order_matrix(transposed):
    here = lax.broadcasted_iota(jnp.int32, (ROWS, ROWS), 1 if transposed else 0)
    position = lax.broadcasted_iota(jnp.int32, (ROWS, ROWS), 0 if transposed else 1)
    return position == (here & (CHUNKS - 1)) * STEPS + (here >> 3)


def softplus_of_minus(rate):
    e = jnp.exp(-jnp.abs(rate))
    series = e * (1 - e * (1 / 2 - e * (1 / 3 - e * (1 / 4 - e * (1 / 5 - e * (1 / 6))))))
    return jnp.maximum(-rate, 0.0) + jnp.where(e < 0.05, series, jnp.log(1.0 + e))


def sublane_before(tile, shift, fill):
    row = lax.broadcasted_iota(jnp.int32, tile.shape, 0)
    return jnp.where(row < shift, fill, pltpu.roll(tile, shift, 0))


def conv_all(x_ref, halo_ref, cw_ref, cv_ref):
    perm = order_matrix(False).astype(bf16)
    for h in range(HEADS):
        cols = pl.ds(h * BLOCK, BLOCK)
        moved = jnp.dot(perm, x_ref[:, cols], preferred_element_type=f32)
        step = [moved[CHUNKS * r : CHUNKS * (r + 1)] for r in range(STEPS)]
        halo = halo_ref[:, cols].astype(f32)
        taps = cw_ref[:, cols].astype(f32)
        early = [
            sublane_before(step[STEPS - j], 1, halo[8 - j : 9 - j]) for j in (3, 2, 1)
        ]
        line = early + step
        for r in range(0, STEPS, 2):
            both = []
            for q in (r, r + 1):
                total = taps[0:1] * line[q]
                for tap in range(1, CONV):
                    total = total + taps[tap : tap + 1] * line[q + tap]
                both.append(total)
            cv_ref[pl.ds(CHUNKS * r, 2 * CHUNKS), cols] = jnp.concatenate(both, 0).astype(bf16)


def one_head(head, cv_ref, w0, w1, pace_ref, rate_ref, pre_ref, h_ref, p_ref, edge_ref, slot):
    cols = pl.ds(pl.multiple_of(head * BLOCK, BLOCK), BLOCK)
    values = cv_ref[:, cols]
    pre_ref[0] = jnp.dot(values, w0, preferred_element_type=f32)
    pre_ref[1] = jnp.dot(values, w1, preferred_element_type=f32)
    pre_ref[2] = values.astype(f32)
    soft = gate_power * softplus_of_minus(rate_ref[:, cols])
    totals = []
    for lane in range(0, BLOCK, LANES):
        at = slice(lane, lane + LANES)
        soft_here = soft[:, at]
        state = run = used = None
        for r in range(STEPS):
            rows = slice(CHUNKS * r, CHUNKS * (r + 1))
            x0 = pre_ref[0, rows, at].astype(bf16).astype(f32)
            x1 = pre_ref[1, rows, at].astype(bf16).astype(f32)
            recur_gate = 1.0 / (1.0 + jnp.exp(-x0))
            input_gate = 1.0 / (1.0 + jnp.exp(-x1))
            loss = pace_ref[rows, :] * recur_gate * soft_here
            decay = jnp.exp(-loss)
            v = 2.0 * loss
            series = v * (1 - v * (1 / 2 - v * (1 / 6 - v * (1 / 24 - v * (1 / 120)))))
            gone = jnp.where(v < 0.1, series, 1.0 - decay * decay)
            drive = jnp.sqrt(gone) * input_gate * pre_ref[2, rows, at]
            if r == 0:
                state, run, used = drive, decay, loss
            else:
                state, run, used = decay * state + drive, decay * run, used + loss
            h_ref[slot, rows, at] = state
            p_ref[slot, rows, at] = run
        for shift in (1, 2, 4):
            state = state + run * sublane_before(state, shift, 0.0)
            run = run * sublane_before(run, shift, 1.0)
        edge_ref[slot, 0, :, at] = sublane_before(state, 1, 0.0)
        edge_ref[slot, 1, :, at] = sublane_before(run, 1, 1.0)
        totals.append((jnp.sum(used, 0, keepdims=True), state[CHUNKS - 1 : CHUNKS]))
    return tuple(jnp.concatenate([t[k] for t in totals], 1) for k in (0, 1))


def place():
    x, c = lax.axis_index("dp_0"), lax.axis_index("dp_1")
    return x, c, (x + 3 + 2 * c) & 3, (x + 1 + 2 * c) & 3, (x + 2) & 3


def heads_of(group):
    x, c, first, second, far = place()
    return {
        "own": [2 * x + c, 2 * first + c, 2 * second + c],
        "mid": [2 * far + c, 2 * x + 1 - c, 2 * second + 1 - c, 2 * first + 1 - c],
        "end": [2 * far + 1 - c],
    }[group]


def own_kernel(x_ref, halo_ref, cw_ref, rate_ref, pace_ref, own_ref, first_ref, second_ref, cv_ref, pcol_ref, pass_ref, h_ref, p_ref, edge_ref, tot_ref, pre_ref):
    here = lax.axis_index("z") * lax.axis_size("y") + lax.axis_index("y")
    pace = pace_ref[:, pl.ds(pl.multiple_of(here * ROWS, ROWS), ROWS)]
    column = jnp.sum(jnp.where(order_matrix(False), pace, 0.0), axis=1, keepdims=True)
    pcol_ref[...] = jnp.broadcast_to(column, (ROWS, LANES))
    conv_all(x_ref, halo_ref, cw_ref, cv_ref)
    maps = (own_ref, first_ref, second_ref)
    for slot, head in enumerate(heads_of("own")):
        pass_ref[slot] = maps[slot][...]
        used, state = one_head(head, cv_ref, maps[slot][0], maps[slot][1], pcol_ref, rate_ref, pre_ref, h_ref, p_ref, edge_ref, slot)
        tot_ref[0, slot : slot + 1] = used
        tot_ref[1, slot : slot + 1] = state


def mid_kernel(cv_ref, pcol_ref, rate_ref, far_ref, swap_ref, h_ref, p_ref, edge_ref, tot_ref, pre_ref):
    for slot, head in enumerate(heads_of("mid")):
        w = far_ref if slot == 0 else swap_ref.at[slot - 1]
        used, state = one_head(head, cv_ref, w[0], w[1], pcol_ref, rate_ref, pre_ref, h_ref, p_ref, edge_ref, slot)
        tot_ref[0, slot : slot + 1] = used
        tot_ref[1, slot : slot + 1] = state


def end_kernel(cv_ref, pcol_ref, rate_ref, w_ref, own_ref, mid_ref, h_ref, p_ref, edge_ref, send_ref, pre_ref):
    (head,) = heads_of("end")
    totals = one_head(head, cv_ref, w_ref[0], w_ref[1], pcol_ref, rate_ref, pre_ref, h_ref, p_ref, edge_ref, 0)
    lines = []
    for k in (0, 1):
        lines += [own_ref[k], mid_ref[k], totals[k]]
    message = jnp.concatenate(lines, 0).astype(bf16)
    for j in range(send_ref.shape[0]):
        send_ref[j] = message


def row_kernel(all_ref, send_ref):
    used = state = None
    for j in range(all_ref.shape[0]):
        line = all_ref[j].astype(f32)
        if j == 0:
            used, state = line[:HEADS], line[HEADS:]
        else:
            used, state = used + line[:HEADS], jnp.exp(-line[:HEADS]) * state + line[HEADS:]
    message = jnp.concatenate([used, state], 0).astype(bf16)
    for j in range(send_ref.shape[0]):
        send_ref[j] = message


def before(all_ref, here, state):
    for j in range(all_ref.shape[0]):
        line = all_ref[j].astype(f32)
        mine = (j < here).astype(f32)
        drive = line[HEADS:] * mine
        state = drive if state is None else jnp.exp(-(line[:HEADS] * mine)) * state + drive
    return state


def last_kernel(row_ref, column_ref, *refs):
    groups, out_ref = refs[:9], refs[9]
    carried = before(column_ref, lax.axis_index("z"), None)
    carried = before(row_ref, lax.axis_index("y"), carried)
    back = order_matrix(True).astype(bf16)
    at = 0
    for g, name in enumerate(("own", "mid", "end")):
        h_ref, p_ref, edge_ref = groups[3 * g : 3 * g + 3]
        for slot, head in enumerate(heads_of(name)):
            enters = edge_ref[slot, 0] + edge_ref[slot, 1] * carried[at : at + 1]
            whole = h_ref[slot].reshape(STEPS, CHUNKS, BLOCK) + p_ref[slot].reshape(
                STEPS, CHUNKS, BLOCK
            ) * enters.reshape(1, CHUNKS, BLOCK)
            rounded = whole.reshape(ROWS, BLOCK).astype(bf16)
            cols = pl.ds(pl.multiple_of(head * BLOCK, BLOCK), BLOCK)
            out_ref[:, cols] = jnp.dot(back, rounded, preferred_element_type=f32).astype(bf16)
            at += 1


def vmem(count):
    return [pl.BlockSpec(memory_space=pltpu.VMEM)] * count


def call(kernel, outs, args, scratch=True, us=2.0):
    return pl.pallas_call(
        kernel,
        out_shape=[jax.ShapeDtypeStruct(s, d) for s, d in outs],
        in_specs=vmem(len(args)),
        out_specs=vmem(len(outs)),
        scratch_shapes=[pltpu.VMEM((3, ROWS, BLOCK), f32)] if scratch else [],
        compiler_params=pltpu.CompilerParams(vmem_limit_bytes=16 * 2**20),
        cost_estimate=pl.CostEstimate(
            flops=int(us * 2e8), bytes_accessed=1 << 20, transcendentals=1 << 18
        ),
    )(*args)


def head_outs(n):
    return [((n, ROWS, BLOCK), f32), ((n, ROWS, BLOCK), f32), ((n, 2, CHUNKS, BLOCK), f32)]


def layer(inputs, conv_weight, gate_weight, rate_param, pace):
    x = inputs[0]
    rate = rate_param[None]
    columns, lines = lax.axis_size("z"), lax.axis_size("y")
    dp, sp = ("dp_0", "dp_1"), ("z", "y")

    def along(array, way):
        pairs = [(2 * i + c, 2 * ((i + (way, -way)[c]) % 4) + c) for i in range(4) for c in (0, 1)]
        return lax.ppermute(array, dp, pairs)

    def swapped(array):
        return lax.ppermute(array, "dp_1", [(0, 1), (1, 0)])

    own = gate_weight[:, 0]
    first = along(own, 1)
    second = along(own, -1)
    halo = lax.ppermute(x[ROWS - 8 :], sp, [(i, i + 1) for i in range(columns * lines - 1)])
    far = along(first, 1)
    cv, pcol, ours, *own_out, own_tot = call(
        own_kernel,
        [
            ((ROWS, HEADS * BLOCK), bf16),
            ((ROWS, LANES), f32),
            ((3, 2, BLOCK, BLOCK), bf16),
            *head_outs(3),
            ((2, 3, BLOCK), f32),
        ],
        (x, halo, conv_weight, rate, pace, own, first, second),
    )
    theirs = swapped(ours)
    far_theirs = swapped(far)
    *mid_out, mid_tot = call(mid_kernel, [*head_outs(4), ((2, 4, BLOCK), f32)], (cv, pcol, rate, far, theirs))
    message = ((lines, 2 * HEADS, BLOCK), bf16)
    *end_out, send = call(end_kernel, [*head_outs(1), message], (cv, pcol, rate, far_theirs, own_tot, mid_tot))
    row = lax.all_to_all(send, "y", split_axis=0, concat_axis=0, tiled=True)
    (send,) = call(row_kernel, [((columns, 2 * HEADS, BLOCK), bf16)], (row,), scratch=False)
    column = lax.all_to_all(send, "z", split_axis=0, concat_axis=0, tiled=True)
    (result,) = call(
        last_kernel, [((ROWS, HEADS * BLOCK), bf16)], (row, column, *own_out, *mid_out, *end_out), scratch=False
    )
    return result[None]


def solution(mesh):
    axes = ("z", "y", "dp_0", "dp_1")
    finer = Mesh(mesh.devices.reshape(mesh.shape["sp"] // 8, 8, 4, 2), axes)
    dp, sp = ("dp_0", "dp_1"), ("z", "y")
    in_specs = (P(dp, sp, None), P(), P(None, dp, None, None), P(), P(dp, None))
    out_specs = P(dp, sp, None)
    return jax.shard_map(layer, mesh=finer, in_specs=in_specs, out_specs=out_specs, check_vma=False)
```

```python
import jax
import jax.numpy as jnp
from jax import lax
from jax.experimental import pallas as pl
from jax.experimental.pallas import tpu as pltpu
from jax.sharding import Mesh
from jax.sharding import PartitionSpec as P

HEADS = 8
BLOCK = 256
CONV = 4
ROWS = 128
CHUNKS = 8
STEPS = ROWS // CHUNKS
LANES = 128


gate_power = 8.0
f32, bf16 = jnp.float32, jnp.bfloat16


def order_matrix(transposed):
    here = lax.broadcasted_iota(jnp.int32, (ROWS, ROWS), 1 if transposed else 0)
    position = lax.broadcasted_iota(jnp.int32, (ROWS, ROWS), 0 if transposed else 1)
    return position == (here & (CHUNKS - 1)) * STEPS + (here >> 3)


def softplus_of_minus(rate):
    e = jnp.exp(-jnp.abs(rate))
    series = e * (1 - e * (1 / 2 - e * (1 / 3 - e * (1 / 4 - e * (1 / 5 - e * (1 / 6))))))
    return jnp.maximum(-rate, 0.0) + jnp.where(e < 0.05, series, jnp.log(1.0 + e))


def sublane_before(tile, shift, fill):
    row = lax.broadcasted_iota(jnp.int32, tile.shape, 0)
    return jnp.where(row < shift, fill, pltpu.roll(tile, shift, 0))


def conv_all(moved_ref, halo_ref, cw_ref, cv_ref):
    for h in range(HEADS):
        cols = pl.ds(h * BLOCK, BLOCK)
        step = []
        for r in range(0, STEPS, 2):
            both = moved_ref[pl.ds(CHUNKS * r, 2 * CHUNKS), cols].astype(f32)
            step += [both[:CHUNKS], both[CHUNKS:]]
        halo = halo_ref[:, cols].astype(f32)
        taps = cw_ref[:, cols].astype(f32)
        early = [
            sublane_before(step[STEPS - j], 1, halo[8 - j : 9 - j]) for j in (3, 2, 1)
        ]
        line = early + step
        for r in range(0, STEPS, 2):
            both = []
            for q in (r, r + 1):
                total = taps[0:1] * line[q]
                for tap in range(1, CONV):
                    total = total + taps[tap : tap + 1] * line[q + tap]
                both.append(total)
            cv_ref[pl.ds(CHUNKS * r, 2 * CHUNKS), cols] = jnp.concatenate(both, 0).astype(bf16)


def one_head(head, cv_ref, w0, w1, pace_ref, rate_ref, pre_ref, h_ref, p_ref, edge_ref, slot):
    cols = pl.ds(pl.multiple_of(head * BLOCK, BLOCK), BLOCK)
    values = cv_ref[:, cols]
    pre_ref[0] = jnp.dot(values, w0, preferred_element_type=f32)
    pre_ref[1] = jnp.dot(values, w1, preferred_element_type=f32)
    pre_ref[2] = values.astype(f32)
    soft = gate_power * softplus_of_minus(rate_ref[:, cols])
    totals = []
    for lane in range(0, BLOCK, LANES):
        at = slice(lane, lane + LANES)
        soft_here = soft[:, at]
        state = run = used = None
        for r in range(STEPS):
            rows = slice(CHUNKS * r, CHUNKS * (r + 1))
            x0 = pre_ref[0, rows, at].astype(bf16).astype(f32)
            x1 = pre_ref[1, rows, at].astype(bf16).astype(f32)
            recur_gate = 1.0 / (1.0 + jnp.exp(-x0))
            input_gate = 1.0 / (1.0 + jnp.exp(-x1))
            loss = pace_ref[rows, :] * recur_gate * soft_here
            decay = jnp.exp(-loss)
            v = 2.0 * loss
            series = v * (1 - v * (1 / 2 - v * (1 / 6 - v * (1 / 24 - v * (1 / 120)))))
            gone = jnp.where(v < 0.1, series, 1.0 - decay * decay)
            drive = jnp.sqrt(gone) * input_gate * pre_ref[2, rows, at]
            if r == 0:
                state, run, used = drive, decay, loss
            else:
                state, run, used = decay * state + drive, decay * run, used + loss
            h_ref[slot, rows, at] = state
            p_ref[slot, rows, at] = run
        for shift in (1, 2, 4):
            state = state + run * sublane_before(state, shift, 0.0)
            run = run * sublane_before(run, shift, 1.0)
        edge_ref[slot, 0, :, at] = sublane_before(state, 1, 0.0)
        edge_ref[slot, 1, :, at] = sublane_before(run, 1, 1.0)
        totals.append((jnp.sum(used, 0, keepdims=True), state[CHUNKS - 1 : CHUNKS]))
    return tuple(jnp.concatenate([t[k] for t in totals], 1) for k in (0, 1))


def place():
    x, c = lax.axis_index("dp_0"), lax.axis_index("dp_1")
    return x, c, (x + 3 + 2 * c) & 3, (x + 1 + 2 * c) & 3, (x + 2) & 3


def heads_of(group):
    x, c, first, second, far = place()
    return {
        "own": [2 * x + c, 2 * first + c, 2 * second + c],
        "rest": [2 * far, 2 * far + 1, 2 * x + 1 - c, 2 * second + 1 - c, 2 * first + 1 - c],
    }[group]


def order_kernel(perm_ref):
    perm_ref[...] = order_matrix(False).astype(bf16)


def move_kernel(x_ref, perm_ref, moved_ref, tail_ref):
    tail_ref[...] = x_ref[ROWS - 8 :]
    perm = perm_ref[...]
    for h in range(HEADS):
        cols = pl.ds(h * BLOCK, BLOCK)
        moved_ref[:, cols] = jnp.dot(perm, x_ref[:, cols], preferred_element_type=f32).astype(bf16)


def conv_kernel(moved_ref, halo_ref, cw_ref, own_ref, first_ref, second_ref, cv_ref, pass_ref):
    for slot, w in enumerate((own_ref, first_ref, second_ref)):
        pass_ref[slot] = w[...]
    conv_all(moved_ref, halo_ref, cw_ref, cv_ref)


def own_kernel(cv_ref, rate_ref, pace_ref, own_ref, first_ref, second_ref, pcol_ref, h_ref, p_ref, edge_ref, tot_ref, pre_ref):
    here = lax.axis_index("z") * lax.axis_size("y") + lax.axis_index("y")
    pace = pace_ref[:, pl.ds(pl.multiple_of(here * ROWS, ROWS), ROWS)]
    column = jnp.sum(jnp.where(order_matrix(False), pace, 0.0), axis=1, keepdims=True)
    pcol_ref[...] = jnp.broadcast_to(column, (ROWS, LANES))
    maps = (own_ref, first_ref, second_ref)
    for slot, head in enumerate(heads_of("own")):
        w = maps[slot]
        used, state = one_head(head, cv_ref, w[0], w[1], pcol_ref, rate_ref, pre_ref, h_ref, p_ref, edge_ref, slot)
        tot_ref[0, slot : slot + 1] = used
        tot_ref[1, slot : slot + 1] = state


def rest_kernel(cv_ref, pcol_ref, rate_ref, far_ref, swap_ref, own_ref, h_ref, p_ref, edge_ref, send_ref, pre_ref):
    totals = []
    for slot, head in enumerate(heads_of("rest")):
        w = far_ref.at[slot] if slot < 2 else swap_ref.at[slot - 2]
        totals.append(one_head(head, cv_ref, w[0], w[1], pcol_ref, rate_ref, pre_ref, h_ref, p_ref, edge_ref, slot))
    lines = []
    for k in (0, 1):
        lines += [own_ref[k]] + [t[k] for t in totals]
    message = jnp.concatenate(lines, 0).astype(bf16)
    for j in range(send_ref.shape[0]):
        send_ref[j] = message


def row_kernel(all_ref, send_ref):
    used = state = None
    for j in range(all_ref.shape[0]):
        line = all_ref[j].astype(f32)
        if j == 0:
            used, state = line[:HEADS], line[HEADS:]
        else:
            used, state = used + line[:HEADS], jnp.exp(-line[:HEADS]) * state + line[HEADS:]
    message = jnp.concatenate([used, state], 0).astype(bf16)
    for j in range(send_ref.shape[0]):
        send_ref[j] = message


def before(all_ref, here, state):
    for j in range(all_ref.shape[0]):
        line = all_ref[j].astype(f32)
        mine = (j < here).astype(f32)
        drive = line[HEADS:] * mine
        state = drive if state is None else jnp.exp(-(line[:HEADS] * mine)) * state + drive
    return state


def last_kernel(row_ref, column_ref, *refs):
    groups, out_ref, block_ref, sem = refs[:6], refs[6], refs[7], refs[8]
    carried = before(column_ref, lax.axis_index("z"), None)
    carried = before(row_ref, lax.axis_index("y"), carried)
    back = order_matrix(True).astype(bf16)
    at, copies = 0, []
    for g, name in enumerate(("own", "rest")):
        h_ref, p_ref, edge_ref = groups[3 * g : 3 * g + 3]
        for slot, head in enumerate(heads_of(name)):
            enters = edge_ref[slot, 0] + edge_ref[slot, 1] * carried[at : at + 1]
            whole = h_ref[slot].reshape(STEPS, CHUNKS, BLOCK) + p_ref[slot].reshape(
                STEPS, CHUNKS, BLOCK
            ) * enters.reshape(1, CHUNKS, BLOCK)
            rounded = whole.reshape(ROWS, BLOCK).astype(bf16)
            block_ref[at] = jnp.dot(back, rounded, preferred_element_type=f32).astype(bf16)
            cols = pl.ds(pl.multiple_of(head * BLOCK, BLOCK), BLOCK)
            copies.append(pltpu.make_async_copy(block_ref.at[at], out_ref.at[:, cols], sem.at[at]))
            copies[-1].start()
            at += 1
    for copy in copies:
        copy.wait()


def call(kernel, outs, args, scratch=None, out_space=pltpu.VMEM, us=2.0):
    if scratch is None:
        scratch = [pltpu.VMEM((3, ROWS, BLOCK), f32)]
    return pl.pallas_call(
        kernel,
        out_shape=[jax.ShapeDtypeStruct(s, d) for s, d in outs],
        in_specs=[pl.BlockSpec(memory_space=pltpu.VMEM)] * len(args),
        out_specs=[pl.BlockSpec(memory_space=out_space)] * len(outs),
        scratch_shapes=scratch,
        compiler_params=pltpu.CompilerParams(vmem_limit_bytes=16 * 2**20),
        cost_estimate=pl.CostEstimate(
            flops=int(us * 2e8), bytes_accessed=1 << 20, transcendentals=1 << 18
        ),
    )(*args)


def head_outs(n):
    return [((n, ROWS, BLOCK), f32), ((n, ROWS, BLOCK), f32), ((n, 2, CHUNKS, BLOCK), f32)]


def layer(inputs, conv_weight, gate_weight, rate_param, pace):
    x = inputs[0]
    rate = rate_param[None]
    columns, lines = lax.axis_size("z"), lax.axis_size("y")
    dp, sp = ("dp_0", "dp_1"), ("z", "y")

    def along(array, way):
        pairs = [(2 * i + c, 2 * ((i + (way, -way)[c]) % 4) + c) for i in range(4) for c in (0, 1)]
        return lax.ppermute(array, dp, pairs)

    own = gate_weight[:, 0]
    (perm,) = call(order_kernel, [((ROWS, ROWS), bf16)], (), scratch=[], us=50.0)
    first = along(own, 1)
    second = along(own, -1)
    moved, tail = call(
        move_kernel,
        [((ROWS, HEADS * BLOCK), bf16), ((8, HEADS * BLOCK), bf16)],
        (x, perm),
        scratch=[],
    )
    halo = lax.ppermute(tail, sp, [(i, i + 1) for i in range(columns * lines - 1)])
    far = along(first, 1)
    cv, ours = call(
        conv_kernel,
        [((ROWS, HEADS * BLOCK), bf16), ((3, 2, BLOCK, BLOCK), bf16)],
        (moved, halo, conv_weight, own, first, second),
        scratch=[],
    )
    theirs = lax.ppermute(ours, "dp_1", [(0, 1), (1, 0)])
    pcol, *own_out, own_tot = call(
        own_kernel,
        [((ROWS, LANES), f32), *head_outs(3), ((2, 3, BLOCK), f32)],
        (cv, rate, pace, own, first, second),
    )
    far_pair = lax.all_gather(far, "dp_1")
    message = ((lines, 2 * HEADS, BLOCK), bf16)
    *rest_out, send = call(
        rest_kernel, [*head_outs(5), message], (cv, pcol, rate, far_pair, theirs, own_tot)
    )
    row = lax.all_to_all(send, "y", split_axis=0, concat_axis=0, tiled=True)
    (send,) = call(row_kernel, [((columns, 2 * HEADS, BLOCK), bf16)], (row,), scratch=[])
    column = lax.all_to_all(send, "z", split_axis=0, concat_axis=0, tiled=True)
    (result,) = call(
        last_kernel,
        [((ROWS, HEADS * BLOCK), bf16)],
        (row, column, *own_out, *rest_out),
        scratch=[pltpu.VMEM((HEADS, ROWS, BLOCK), bf16), pltpu.SemaphoreType.DMA((HEADS,))],
        out_space=pl.ANY,
    )
    return result[None]


def solution(mesh):
    axes = ("z", "y", "dp_0", "dp_1")
    finer = Mesh(mesh.devices.reshape(mesh.shape["sp"] // 8, 8, 4, 2), axes)
    dp, sp = ("dp_0", "dp_1"), ("z", "y")
    in_specs = (P(dp, sp, None), P(), P(None, dp, None, None), P(), P(dp, None))
    out_specs = P(dp, sp, None)
    return jax.shard_map(layer, mesh=finer, in_specs=in_specs, out_specs=out_specs, check_vma=False)
```

```python
import jax
import jax.numpy as jnp
from jax import lax
from jax.experimental import pallas as pl
from jax.experimental.pallas import tpu as pltpu
from jax.sharding import Mesh
from jax.sharding import PartitionSpec as P

HEADS = 8
BLOCK = 256
CONV = 4
ROWS = 128
CHUNKS = 8
STEPS = ROWS // CHUNKS
LANES = 128


LOG2E = 1.4426950408889634
LEAST = 1.1754944e-38
gate_power = 8.0
f32, bf16 = jnp.float32, jnp.bfloat16


def order_matrix(transposed):
    here = lax.broadcasted_iota(jnp.int32, (ROWS, ROWS), 1 if transposed else 0)
    position = lax.broadcasted_iota(jnp.int32, (ROWS, ROWS), 0 if transposed else 1)
    return position == (here & (CHUNKS - 1)) * STEPS + (here >> 3)


def softplus_of_minus(rate):
    e = jnp.exp(-jnp.abs(rate))
    series = e * (1 - e * (1 / 2 - e * (1 / 3 - e * (1 / 4 - e * (1 / 5 - e * (1 / 6))))))
    return jnp.maximum(-rate, 0.0) + jnp.where(e < 0.05, series, jnp.log(1.0 + e))


def sublane_before(tile, shift, fill):
    row = lax.broadcasted_iota(jnp.int32, tile.shape, 0)
    return jnp.where(row < shift, fill, pltpu.roll(tile, shift, 0))


def conv_all(moved_ref, halo_ref, cw_ref, cv_ref):
    for h in range(HEADS):
        cols = pl.ds(h * BLOCK, BLOCK)
        step = []
        for r in range(0, STEPS, 2):
            both = moved_ref[pl.ds(CHUNKS * r, 2 * CHUNKS), cols].astype(f32)
            step += [both[:CHUNKS], both[CHUNKS:]]
        halo = halo_ref[:, cols].astype(f32)
        taps = cw_ref[:, cols].astype(f32)
        early = [
            sublane_before(step[STEPS - j], 1, halo[8 - j : 9 - j]) for j in (3, 2, 1)
        ]
        line = early + step
        for r in range(0, STEPS, 2):
            both = []
            for q in (r, r + 1):
                total = taps[0:1] * line[q]
                for tap in range(1, CONV):
                    total = total + taps[tap : tap + 1] * line[q + tap]
                both.append(total)
            cv_ref[pl.ds(CHUNKS * r, 2 * CHUNKS), cols] = jnp.concatenate(both, 0).astype(bf16)


def one_head(head, cv_ref, w0, w1, pace_ref, rate_ref, pre_ref, h_ref, p_ref, edge_ref, slot):
    cols = pl.ds(pl.multiple_of(head * BLOCK, BLOCK), BLOCK)
    values = cv_ref[:, cols]
    pre_ref[0] = jnp.dot(values, w0, preferred_element_type=f32)
    pre_ref[1] = jnp.dot(values, w1, preferred_element_type=f32)
    pre_ref[2] = values.astype(f32)
    soft = 2.0 * gate_power * softplus_of_minus(rate_ref[:, cols])
    totals = []
    for lane in range(0, BLOCK, LANES):
        at = slice(lane, lane + LANES)
        soft_here = soft[:, at]
        state = run = used = None
        for r in range(STEPS):
            rows = slice(CHUNKS * r, CHUNKS * (r + 1))
            x0 = pre_ref[0, rows, at].astype(bf16).astype(f32)
            x1 = pre_ref[1, rows, at].astype(bf16).astype(f32)
            recur_gate = 1.0 / (1.0 + jnp.exp2(x0 * -LOG2E))
            input_gate = 1.0 / (1.0 + jnp.exp2(x1 * -LOG2E))
            v = pace_ref[rows, :] * recur_gate * soft_here
            decay = jnp.exp2(v * (-0.5 * LOG2E))
            series = v * (1 - v * (1 / 2 - v * (1 / 6 - v * (1 / 24))))
            gone = jnp.where(v < 0.03, series, 1.0 - decay * decay)
            root = gone * lax.rsqrt(jnp.maximum(gone, LEAST))
            drive = root * input_gate * pre_ref[2, rows, at]
            if r == 0:
                state, run, used = drive, decay, v
            else:
                state, run, used = decay * state + drive, decay * run, used + v
            h_ref[slot, rows, at] = state
            p_ref[slot, rows, at] = run
        for shift in (1, 2, 4):
            state = state + run * sublane_before(state, shift, 0.0)
            run = run * sublane_before(run, shift, 1.0)
        edge_ref[slot, 0, :, at] = sublane_before(state, 1, 0.0)
        edge_ref[slot, 1, :, at] = sublane_before(run, 1, 1.0)
        totals.append((0.5 * jnp.sum(used, 0, keepdims=True), state[CHUNKS - 1 : CHUNKS]))
    return tuple(jnp.concatenate([t[k] for t in totals], 1) for k in (0, 1))


def place():
    x, c = lax.axis_index("dp_0"), lax.axis_index("dp_1")
    return x, c, (x + 3 + 2 * c) & 3, (x + 1 + 2 * c) & 3, (x + 2) & 3


def heads_of(group):
    x, c, first, second, far = place()
    return {
        "own": [2 * x + c, 2 * first + c, 2 * second + c],
        "rest": [2 * far, 2 * far + 1, 2 * x + 1 - c, 2 * second + 1 - c, 2 * first + 1 - c],
    }[group]


def order_kernel(perm_ref):
    perm_ref[...] = order_matrix(False).astype(bf16)


def move_kernel(x_ref, perm_ref, moved_ref, tail_ref):
    tail_ref[...] = x_ref[ROWS - 8 :]
    perm = perm_ref[...]
    for h in range(HEADS):
        cols = pl.ds(h * BLOCK, BLOCK)
        moved_ref[:, cols] = jnp.dot(perm, x_ref[:, cols], preferred_element_type=f32).astype(bf16)


def conv_kernel(moved_ref, halo_ref, cw_ref, own_ref, first_ref, second_ref, cv_ref, pass_ref):
    for slot, w in enumerate((own_ref, first_ref, second_ref)):
        pass_ref[slot] = w[...]
    conv_all(moved_ref, halo_ref, cw_ref, cv_ref)


def own_kernel(cv_ref, rate_ref, pace_ref, own_ref, first_ref, second_ref, pcol_ref, h_ref, p_ref, edge_ref, tot_ref, pre_ref):
    here = lax.axis_index("z") * lax.axis_size("y") + lax.axis_index("y")
    pace = pace_ref[:, pl.ds(pl.multiple_of(here * ROWS, ROWS), ROWS)]
    column = jnp.sum(jnp.where(order_matrix(False), pace, 0.0), axis=1, keepdims=True)
    pcol_ref[...] = jnp.broadcast_to(column, (ROWS, LANES))
    maps = (own_ref, first_ref, second_ref)
    for slot, head in enumerate(heads_of("own")):
        w = maps[slot]
        used, state = one_head(head, cv_ref, w[0], w[1], pcol_ref, rate_ref, pre_ref, h_ref, p_ref, edge_ref, slot)
        tot_ref[0, slot : slot + 1] = used
        tot_ref[1, slot : slot + 1] = state


def rest_kernel(cv_ref, pcol_ref, rate_ref, far_ref, swap_ref, own_ref, h_ref, p_ref, edge_ref, send_ref, pre_ref):
    totals = []
    for slot, head in enumerate(heads_of("rest")):
        w = far_ref.at[slot] if slot < 2 else swap_ref.at[slot - 2]
        totals.append(one_head(head, cv_ref, w[0], w[1], pcol_ref, rate_ref, pre_ref, h_ref, p_ref, edge_ref, slot))
    lines = []
    for k in (0, 1):
        lines += [own_ref[k]] + [t[k] for t in totals]
    message = jnp.concatenate(lines, 0).astype(bf16)
    for j in range(send_ref.shape[0]):
        send_ref[j] = message


def row_kernel(all_ref, send_ref):
    used = state = None
    for j in range(all_ref.shape[0]):
        line = all_ref[j].astype(f32)
        if j == 0:
            used, state = line[:HEADS], line[HEADS:]
        else:
            used, state = used + line[:HEADS], jnp.exp(-line[:HEADS]) * state + line[HEADS:]
    message = jnp.concatenate([used, state], 0).astype(bf16)
    for j in range(send_ref.shape[0]):
        send_ref[j] = message


def before(all_ref, here, state):
    for j in range(all_ref.shape[0]):
        line = all_ref[j].astype(f32)
        mine = (j < here).astype(f32)
        drive = line[HEADS:] * mine
        state = drive if state is None else jnp.exp(-(line[:HEADS] * mine)) * state + drive
    return state


def last_kernel(row_ref, column_ref, *refs):
    groups, out_ref, block_ref, sem = refs[:6], refs[6], refs[7], refs[8]
    carried = before(column_ref, lax.axis_index("z"), None)
    carried = before(row_ref, lax.axis_index("y"), carried)
    back = order_matrix(True).astype(bf16)
    at, copies = 0, []
    for g, name in enumerate(("own", "rest")):
        h_ref, p_ref, edge_ref = groups[3 * g : 3 * g + 3]
        for slot, head in enumerate(heads_of(name)):
            enters = edge_ref[slot, 0] + edge_ref[slot, 1] * carried[at : at + 1]
            whole = h_ref[slot].reshape(STEPS, CHUNKS, BLOCK) + p_ref[slot].reshape(
                STEPS, CHUNKS, BLOCK
            ) * enters.reshape(1, CHUNKS, BLOCK)
            rounded = whole.reshape(ROWS, BLOCK).astype(bf16)
            block_ref[at] = jnp.dot(back, rounded, preferred_element_type=f32).astype(bf16)
            cols = pl.ds(pl.multiple_of(head * BLOCK, BLOCK), BLOCK)
            copies.append(pltpu.make_async_copy(block_ref.at[at], out_ref.at[:, cols], sem.at[at]))
            copies[-1].start()
            at += 1
    for copy in copies:
        copy.wait()


def call(kernel, outs, args, scratch=None, out_space=pltpu.VMEM, us=2.0):
    if scratch is None:
        scratch = [pltpu.VMEM((3, ROWS, BLOCK), f32)]
    return pl.pallas_call(
        kernel,
        out_shape=[jax.ShapeDtypeStruct(s, d) for s, d in outs],
        in_specs=[pl.BlockSpec(memory_space=pltpu.VMEM)] * len(args),
        out_specs=[pl.BlockSpec(memory_space=out_space)] * len(outs),
        scratch_shapes=scratch,
        compiler_params=pltpu.CompilerParams(vmem_limit_bytes=16 * 2**20),
        cost_estimate=pl.CostEstimate(
            flops=int(us * 2e8), bytes_accessed=1 << 20, transcendentals=1 << 18
        ),
    )(*args)


def head_outs(n):
    return [((n, ROWS, BLOCK), f32), ((n, ROWS, BLOCK), f32), ((n, 2, CHUNKS, BLOCK), f32)]


def layer(inputs, conv_weight, gate_weight, rate_param, pace):
    x = inputs[0]
    rate = rate_param[None]
    columns, lines = lax.axis_size("z"), lax.axis_size("y")
    dp, sp = ("dp_0", "dp_1"), ("z", "y")

    def along(array, way):
        pairs = [(2 * i + c, 2 * ((i + (way, -way)[c]) % 4) + c) for i in range(4) for c in (0, 1)]
        return lax.ppermute(array, dp, pairs)

    own = gate_weight[:, 0]
    (perm,) = call(order_kernel, [((ROWS, ROWS), bf16)], (), scratch=[], us=50.0)
    first = along(own, 1)
    second = along(own, -1)
    moved, tail = call(
        move_kernel,
        [((ROWS, HEADS * BLOCK), bf16), ((8, HEADS * BLOCK), bf16)],
        (x, perm),
        scratch=[],
    )
    halo = lax.ppermute(tail, sp, [(i, i + 1) for i in range(columns * lines - 1)])
    far = along(first, 1)
    cv, ours = call(
        conv_kernel,
        [((ROWS, HEADS * BLOCK), bf16), ((3, 2, BLOCK, BLOCK), bf16)],
        (moved, halo, conv_weight, own, first, second),
        scratch=[],
    )
    theirs = lax.ppermute(ours, "dp_1", [(0, 1), (1, 0)])
    pcol, *own_out, own_tot = call(
        own_kernel,
        [((ROWS, LANES), f32), *head_outs(3), ((2, 3, BLOCK), f32)],
        (cv, rate, pace, own, first, second),
    )
    far_pair = lax.all_gather(far, "dp_1")
    message = ((lines, 2 * HEADS, BLOCK), bf16)
    *rest_out, send = call(
        rest_kernel, [*head_outs(5), message], (cv, pcol, rate, far_pair, theirs, own_tot)
    )
    row = lax.all_to_all(send, "y", split_axis=0, concat_axis=0, tiled=True)
    (send,) = call(row_kernel, [((columns, 2 * HEADS, BLOCK), bf16)], (row,), scratch=[])
    column = lax.all_to_all(send, "z", split_axis=0, concat_axis=0, tiled=True)
    (result,) = call(
        last_kernel,
        [((ROWS, HEADS * BLOCK), bf16)],
        (row, column, *own_out, *rest_out),
        scratch=[pltpu.VMEM((HEADS, ROWS, BLOCK), bf16), pltpu.SemaphoreType.DMA((HEADS,))],
        out_space=pl.ANY,
    )
    return result[None]


def solution(mesh):
    axes = ("z", "y", "dp_0", "dp_1")
    finer = Mesh(mesh.devices.reshape(mesh.shape["sp"] // 8, 8, 4, 2), axes)
    dp, sp = ("dp_0", "dp_1"), ("z", "y")
    in_specs = (P(dp, sp, None), P(), P(None, dp, None, None), P(), P(dp, None))
    out_specs = P(dp, sp, None)
    return jax.shard_map(layer, mesh=finer, in_specs=in_specs, out_specs=out_specs, check_vma=False)
```
